32 devices in a mesh: sp: 8 (over z, y), dp: 4 (over x, core).
Axes of the slice: x: 2, y: 2, z: 4, core: 2. Of those that a mesh axis runs over, the one named last changes fastest.
Arguments:
- tokens: bfloat16 [4, 2048, 2048], P('dp', 'sp'), may hold values from -6 to 6
- w_query: bfloat16 [2048, 2048], P('dp', 'sp'), may hold values from -0.125 to 0.125
- w_key: bfloat16 [2048, 1024], P('dp', 'sp'), may hold values from -0.125 to 0.125
- w_value: bfloat16 [2048, 1024], P('dp', 'sp'), may hold values from -0.125 to 0.125
- w_out: bfloat16 [2048, 2048], P('dp', 'sp'), may hold values from -0.25 to 0.25
- qk_gain: float32 [2, 128], replicated, may hold values from 0.9 to 24
Outputs:
- mixed_out: bfloat16 [4, 2048, 2048], P('dp', 'sp')
The draws below stay inside these ranges and needn't reach their ends.
All inputs are finite; a program needn't handle non-finite values.
Results may differ from the reference program's by a relative error of at most 0.006.
The reference program's roundings to bfloat16 on the way count: a program that leaves them out, or rounds other values in their place, can miss the bound.
Values may be sent and summed in bfloat16 or wider, within the bound.
A program may use at most 64 MiB of HBM per device.

```python
import math
import jax
import jax.numpy as jnp
from jax import lax

D = 2048
HQ = 16
KV = 8
HD = 128
GRID_W = 64
SEQ = 2048
SEQS = 4


def draw_qk_gain(key, part):
    noise = jnp.clip(jax.random.normal(key, (2, HD), jnp.float32), -3.0, 3.0)
    return 2.0 * (1.0 + 0.18 * noise)


def steps_of(rng, shape, split, low, largest):
    def one(dim, parts):
        heights = jax.random.uniform(jax.random.fold_in(jax.random.fold_in(rng, 6), dim), (parts,), jnp.float32, low / len(split), largest / len(split))
        return jnp.repeat(jnp.exp(heights), shape[dim] // parts).reshape((-1,) + (1,) * (len(shape) - dim - 1))

    level = one(*split[0])
    for cut in split[1:]:
        level = level * one(*cut)
    return level


def normal_values(key, extent, width, limit, cuts=(), held_as=jnp.bfloat16):
    result = jax.random.normal(key, extent, jnp.float32) * width
    if len(cuts) > 0:
        result = steps_of(key, extent, cuts, -0.22, 0.18) * result
    return jnp.clip(result, min=-limit, max=limit).astype(held_as)


def setup_inputs(seed: int = 0) -> dict:
    streams_of = jax.random.split(jax.random.key(seed), 7)
    tokens = normal_values(streams_of[0], (SEQS, SEQ, D), 1.0, 6.0, ((0, 4), (1, 8)))
    w_query = normal_values(streams_of[1], (D, HQ * HD), D ** -0.5, 0.125, ((0, 4), (1, 8)))
    w_key = normal_values(streams_of[2], (D, KV * HD), D ** -0.5, 0.125, ((0, 4), (1, 8)))
    w_value = normal_values(streams_of[3], (D, KV * HD), D ** -0.5, 0.125, ((0, 4), (1, 8)))
    w_out = normal_values(streams_of[4], (HQ * HD, D), (HQ * HD // 4) ** -0.5, 0.25, ((0, 4), (1, 8)))
    qk_gain = draw_qk_gain(jax.random.fold_in(streams_of[6], 71), 0)
    return dict(tokens=tokens, w_query=w_query, w_key=w_key, w_value=w_value, w_out=w_out, qk_gain=qk_gain)


ROPE_BASE = 10000.0
EPS = 1e-06

def angles(positions):
    quarter = jnp.arange(0, HD // 2, 2, dtype=jnp.float32)
    inv_freq = ROPE_BASE ** (-quarter / (HD // 2))
    row_pos = (positions // GRID_W).astype(jnp.float32)
    col_pos = (positions % GRID_W).astype(jnp.float32)
    angle_table = jnp.concatenate([row_pos[:, None] * inv_freq, col_pos[:, None] * inv_freq], axis=1)
    return (jnp.cos(angle_table), jnp.sin(angle_table))

def prepare(raw_proj, gain_row, cosine, sine_table):
    normed = raw_proj * lax.rsqrt(lax.optimization_barrier(jnp.mean(raw_proj * raw_proj, axis=-1, keepdims=True)) + EPS) * gain_row
    pair_view = normed.reshape(raw_proj.shape[:-1] + (HD // 2, 2))
    first_half = pair_view[..., 0]
    second = pair_view[..., 1]
    cos_b = cosine[:, None, :]
    sin_b = sine_table[:, None, :]
    turned = jnp.stack([first_half * cos_b - second * sin_b, first_half * sin_b + second * cos_b], axis=-1)
    return turned.reshape(raw_proj.shape).astype(jnp.bfloat16)

def attend_head(query_rows, key_rows, value_rows):
    seq_len = query_rows.shape[0]
    block_len = math.gcd(seq_len, 512)
    blocks = query_rows.reshape(seq_len // block_len, block_len, HD)

    def one_block(row_block):
        scores = jnp.dot(row_block, key_rows.T, preferred_element_type=jnp.float32) * HD ** (-0.5)
        top_score = lax.optimization_barrier(jnp.max(scores, axis=1, keepdims=True))
        weights = jnp.exp(scores - top_score)
        row_total = lax.optimization_barrier(jnp.sum(weights, axis=1, keepdims=True))
        probs_bf = (weights / row_total).astype(jnp.bfloat16)
        return jnp.dot(probs_bf, value_rows, preferred_element_type=jnp.float32).astype(jnp.bfloat16)
    return lax.map(one_block, blocks).reshape(seq_len, HD)

def reference(tokens, w_query, w_key, w_value, w_out, qk_gain):
    seq_len = tokens.shape[1]
    group_size = HQ // KV
    cosine, sine_table = angles(jnp.arange(seq_len, dtype=jnp.int32))

    def one_sequence(seq_rows):
        query = prepare(jnp.dot(seq_rows, w_query, preferred_element_type=jnp.float32).reshape(seq_len, HQ, HD), qk_gain[0], cosine, sine_table)
        key_all = prepare(jnp.dot(seq_rows, w_key, preferred_element_type=jnp.float32).reshape(seq_len, KV, HD), qk_gain[1], cosine, sine_table)
        value = jnp.dot(seq_rows, w_value, preferred_element_type=jnp.float32).astype(jnp.bfloat16).reshape(seq_len, KV, HD)
        query_heads = jnp.transpose(query, (1, 0, 2))
        key_heads = jnp.repeat(jnp.transpose(key_all, (1, 0, 2)), group_size, axis=0)
        value_heads = jnp.repeat(jnp.transpose(value, (1, 0, 2)), group_size, axis=0)
        attended = lax.map(lambda triple: attend_head(triple[0], triple[1], triple[2]), (query_heads, key_heads, value_heads))
        attended = jnp.transpose(attended, (1, 0, 2)).reshape(seq_len, HQ * HD)
        return jnp.dot(attended, w_out, preferred_element_type=jnp.float32).astype(jnp.bfloat16)
    return lax.map(one_sequence, tokens)
```

```python
import functools

import jax
import jax.numpy as jnp
from jax import lax
from jax.experimental import pallas as pl
from jax.experimental.pallas import tpu as pltpu
from jax.sharding import PartitionSpec as P

HQ = 16
KV = 8
HD = 128
GRID_W = 64
ROPE_BASE = 10000.0
EPS = 1e-06
LOG2E = 1.4426950408889634
VMEM_CAP = 60 * 1024 * 1024


def rope_tables(seq_len):
    quarter = jnp.arange(0, HD // 2, 2, dtype=jnp.float32)
    inv_freq = jnp.repeat(ROPE_BASE ** (-quarter / (HD // 2)), 2)
    rows = jnp.arange(seq_len // GRID_W, dtype=jnp.int32).astype(jnp.float32)
    cols = jnp.arange(GRID_W, dtype=jnp.int32).astype(jnp.float32)
    row_angle = rows[:, None] * inv_freq
    col_angle = cols[:, None] * inv_freq
    sign = jnp.where(jnp.arange(HD // 2) % 2 == 0, -1.0, 1.0).astype(jnp.float32)

    def table(fn):
        by_row = jnp.broadcast_to(fn(row_angle)[:, None, :], (seq_len // GRID_W, GRID_W, HD // 2))
        by_col = jnp.broadcast_to(fn(col_angle)[None, :, :], (seq_len // GRID_W, GRID_W, HD // 2))
        return jnp.concatenate([by_row, by_col], axis=2).reshape(seq_len, HD)

    return table(jnp.cos), table(lambda a: jnp.sin(a) * sign)


def attention_kernel(
    nb, tb, tq, hq, hk, x_ref, w_ref, cos_ref, sin_ref, gain_ref, o_ref, q_s, k_s, v_s
):
    i = pl.program_id(0)

    @pl.when(i < nb)
    def _():
        raw = jnp.dot(x_ref[...], w_ref[...], preferred_element_type=jnp.float32)
        cosine = cos_ref[...]
        sine = sin_ref[...]
        even = lax.broadcasted_iota(jnp.int32, (tb, HD), 1) % 2 == 0
        rows = pl.ds(pl.multiple_of(i * tb, tb), tb)
        for h in range(hq + hk):
            r = raw[:, h * HD : (h + 1) * HD]
            gain = gain_ref[0:1, :] if h < hq else gain_ref[1:2, :]
            n = r * lax.rsqrt(jnp.mean(r * r, axis=-1, keepdims=True) + EPS) * gain
            swapped = jnp.where(even, pltpu.roll(n, HD - 1, 1), pltpu.roll(n, 1, 1))
            turned = (n * cosine + swapped * sine).astype(jnp.bfloat16)
            if h < hq:
                q_s[h, rows, :] = turned
            else:
                k_s[h - hq, rows, :] = turned
        for h in range(hk):
            v_s[h, rows, :] = raw[:, (hq + hk + h) * HD : (hq + hk + h + 1) * HD].astype(
                jnp.bfloat16
            )

    @pl.when(i >= nb)
    def _():
        rows = pl.ds(pl.multiple_of((i - nb) * tq, tq), tq)
        c = HD ** (-0.5) * LOG2E
        for h in range(hq):
            g = h * hk // hq
            s = lax.dot_general(
                q_s[h, rows, :],
                k_s[g],
                (((1,), (1,)), ((), ())),
                preferred_element_type=jnp.float32,
            )
            p = jnp.exp2((s - jnp.max(s, axis=1, keepdims=True)) * c)
            inv = 1.0 / jnp.sum(p, axis=1, keepdims=True)
            probs = (p * inv).astype(jnp.bfloat16)
            o_ref[:, h * HD : (h + 1) * HD] = jnp.dot(
                probs, v_s[g], preferred_element_type=jnp.float32
            ).astype(jnp.bfloat16)


def attend(seq_rows, weights, cosine, sine, gain, hq, hk):
    seq_len, width = seq_rows.shape
    tb = min(512, seq_len)
    tq = min(256, seq_len)
    nb, nq = seq_len // tb, seq_len // tq
    block = lambda i: (jnp.minimum(i, nb - 1), 0)
    whole = lambda i: (0, 0)
    return pl.pallas_call(
        functools.partial(attention_kernel, nb, tb, tq, hq, hk),
        grid=(nb + nq,),
        out_shape=jax.ShapeDtypeStruct((seq_len, hq * HD), jnp.bfloat16),
        in_specs=[
            pl.BlockSpec((tb, width), block),
            pl.BlockSpec(weights.shape, whole),
            pl.BlockSpec((tb, HD), block),
            pl.BlockSpec((tb, HD), block),
            pl.BlockSpec(gain.shape, whole),
        ],
        out_specs=pl.BlockSpec((tq, hq * HD), lambda i: (jnp.maximum(i - nb, 0), 0)),
        scratch_shapes=[
            pltpu.VMEM((hq, seq_len, HD), jnp.bfloat16),
            pltpu.VMEM((hk, seq_len, HD), jnp.bfloat16),
            pltpu.VMEM((hk, seq_len, HD), jnp.bfloat16),
        ],
        compiler_params=pltpu.CompilerParams(vmem_limit_bytes=VMEM_CAP),
        cost_estimate=pl.CostEstimate(
            flops=2 * seq_len * width * weights.shape[1] + 4 * hq * seq_len * seq_len * HD,
            bytes_accessed=2 * (seq_rows.size + weights.size),
            transcendentals=hq * seq_len * seq_len,
        ),
    )(seq_rows, weights, cosine, sine, gain)


def mix_kernel(a_ref, w_ref, o_ref):
    n_src, tok, feat = a_ref.shape
    per = w_ref.shape[2] // feat
    total = None
    for s in range(n_src):
        term = jnp.dot(
            a_ref[s],
            w_ref[s // per, 0, (s % per) * feat : (s % per + 1) * feat, :],
            preferred_element_type=jnp.float32,
        )
        total = term if total is None else total + term
    o_ref[...] = total.astype(o_ref.dtype)


def mix(attended, w_all):
    n_src, tok, feat = attended.shape
    n_dp, n_sp, depth, cols = w_all.shape
    return pl.pallas_call(
        mix_kernel,
        grid=(n_sp,),
        out_shape=jax.ShapeDtypeStruct((tok, n_sp * cols), jnp.bfloat16),
        in_specs=[
            pl.BlockSpec(attended.shape, lambda s: (0, 0, 0)),
            pl.BlockSpec((n_dp, 1, depth, cols), lambda s: (0, s, 0, 0)),
        ],
        out_specs=pl.BlockSpec((tok, cols), lambda s: (0, s)),
        compiler_params=pltpu.CompilerParams(vmem_limit_bytes=VMEM_CAP),
        cost_estimate=pl.CostEstimate(
            flops=2 * tok * w_all.size, bytes_accessed=2 * w_all.size, transcendentals=0
        ),
    )(attended, w_all)


def head_columns(weight, n_sp):
    local = weight.shape[1]
    if local >= HD:
        return weight
    group = HD // local
    groups = [list(range(g, g + group)) for g in range(0, n_sp, group)]
    return lax.all_gather(weight, "sp", axis=1, tiled=True, axis_index_groups=groups)


def on_device(tokens, w_query, w_key, w_value, w_out, qk_gain):
    n_sp = lax.axis_size("sp")
    n_dp = lax.axis_size("dp")
    own_rows = tokens[0]
    tok = own_rows.shape[0]
    seq_len = tok * n_sp
    hq = HQ // n_sp
    hk = max(1, KV // n_sp)
    cosine, sine = rope_tables(seq_len)
    w_local = jnp.concatenate(
        [w_query, head_columns(w_key, n_sp), head_columns(w_value, n_sp)], axis=1
    )
    weights = lax.all_gather(w_local, "dp", axis=0, tiled=True)
    seq_rows = lax.all_gather(own_rows, "sp", axis=0, tiled=True)
    w_all = lax.all_gather(w_out, ("dp", "sp"), axis=0, tiled=False)
    w_all = w_all.reshape((n_dp, n_sp) + w_out.shape)
    attended = attend(seq_rows, weights, cosine, sine, qk_gain, hq, hk)
    blocks = lax.all_to_all(
        attended.reshape(n_sp, tok, hq * HD), "sp", split_axis=0, concat_axis=0, tiled=True
    )
    return mix(blocks, w_all)[None]


def solution(mesh):
    in_specs = (
        P("dp", "sp", None),
        P("dp", "sp"),
        P("dp", "sp"),
        P("dp", "sp"),
        P("dp", "sp"),
        P(),
    )
    return jax.shard_map(
        on_device, mesh=mesh, in_specs=in_specs, out_specs=P("dp", "sp", None), check_vma=False
    )
```

```python
import functools

import jax
import jax.numpy as jnp
from jax import lax
from jax.experimental import pallas as pl
from jax.experimental.pallas import tpu as pltpu
from jax.sharding import PartitionSpec as P

HQ = 16
KV = 8
HD = 128
GRID_W = 64
ROPE_BASE = 10000.0
EPS = 1e-06
LOG2E = 1.4426950408889634
VMEM_CAP = 60 * 1024 * 1024


MESH = pl.DeviceIdType.MESH


def rope_tables(seq_len):
    quarter = jnp.arange(0, HD // 2, 2, dtype=jnp.float32)
    inv_freq = jnp.repeat(ROPE_BASE ** (-quarter / (HD // 2)), 2)
    inv_freq = jnp.concatenate([inv_freq, inv_freq])
    count = max(GRID_W, seq_len // GRID_W)
    angle = jnp.arange(count, dtype=jnp.int32).astype(jnp.float32)[:, None] * inv_freq
    sign = jnp.where(jnp.arange(HD) % 2 == 0, -1.0, 1.0).astype(jnp.float32)
    return jnp.cos(angle), jnp.sin(angle) * sign


def layer_kernel(
    n_sp, n_dp, hq, hk,
    tok_ref, wq_ref, wk_ref, wv_ref, wo_ref, cos_ref, sin_ref, gain_ref,
    out_ref,
    x_all, w_all, wo_all, q_s, k_s, v_s, att_s, att_all,
    local_sem, ring_send, ring_recv, w_send, w_recv, wo_send, wo_recv, att_send, att_recv,
):
    tok = tok_ref.shape[0]
    half = n_sp // 2
    me = lax.axis_index("sp")
    dp = lax.axis_index("dp")
    pos = me // 2 + (me % 2) * (n_sp - 1 - 2 * (me // 2))

    def at_pos(p):
        p = lax.rem(p + 2 * n_sp, n_sp)
        return 2 * p + (p // half) * (2 * (n_sp - 1 - p) + 1 - 2 * p)

    q_cols, k_cols = wq_ref.shape[1], wk_ref.shape[1]
    mine = w_all.at[dp]
    loads = [
        (tok_ref, x_all.at[me]),
        (wo_ref, wo_all.at[dp, me]),
        (wq_ref, mine.at[:, 0:q_cols]),
        (wk_ref, mine.at[:, q_cols : q_cols + k_cols]),
        (wv_ref, mine.at[:, q_cols + k_cols : q_cols + 2 * k_cols]),
    ]
    loads = [pltpu.make_async_copy(a, b, local_sem.at[i]) for i, (a, b) in enumerate(loads)]
    for load in loads:
        load.start()

    barrier = pltpu.get_barrier_semaphore()
    for r in range(1, n_sp):
        pl.semaphore_signal(
            barrier, inc=1, device_id={"sp": lax.rem(me + r, n_sp)}, device_id_type=MESH
        )
    for r in range(1, n_dp):
        pl.semaphore_signal(
            barrier, inc=1, device_id={"dp": lax.rem(dp + r, n_dp)}, device_id_type=MESH
        )
    pl.semaphore_wait(barrier, n_sp - 1 + n_dp - 1)
    for load in loads:
        load.wait()

    def ring_copy(way, part, kind, slot, t):
        if kind == 0:
            rows = tok // 2
            ref = x_all.at[slot, part * rows : (part + 1) * rows]
        else:
            rows = wo_all.shape[2] // 2
            ref = wo_all.at[dp, slot, part * rows : (part + 1) * rows]
        return pltpu.make_async_remote_copy(
            src_ref=ref,
            dst_ref=ref,
            send_sem=ring_send.at[way, part, kind, t],
            recv_sem=ring_recv.at[way, part, kind, t],
            device_id={"sp": at_pos(pos + 1 - 2 * way)},
            device_id_type=MESH,
        )

    def slot_at(way, distance):
        return at_pos(pos - (1 - 2 * way) * distance)

    def w_copy(r, source):
        return pltpu.make_async_remote_copy(
            src_ref=w_all.at[source],
            dst_ref=w_all.at[source],
            send_sem=w_send.at[r - 1],
            recv_sem=w_recv.at[r - 1],
            device_id={"dp": lax.rem(dp + r, n_dp)},
            device_id_type=MESH,
        )

    def wo_copy(r, source, slot):
        return pltpu.make_async_remote_copy(
            src_ref=wo_all.at[source, slot],
            dst_ref=wo_all.at[source, slot],
            send_sem=wo_send.at[r - 1, slot],
            recv_sem=wo_recv.at[r - 1, slot],
            device_id={"dp": lax.rem(dp + r, n_dp)},
            device_id_type=MESH,
        )

    def spread(slot):
        for r in range(1, n_dp):
            wo_copy(r, dp, slot).start()

    def project(slot):
        raw = jnp.dot(
            x_all[slot],
            w_all[...].reshape(w_all.shape[0] * w_all.shape[1], w_all.shape[2]),
            preferred_element_type=jnp.float32,
        )
        lanes = lax.broadcasted_iota(jnp.int32, (GRID_W, HD), 1)
        grid_rows = tok // GRID_W

        def table(ref):
            parts = []
            for g in range(grid_rows):
                row = ref[pl.ds(slot * grid_rows + g, 1), :]
                parts.append(
                    jnp.where(lanes < HD // 2, jnp.broadcast_to(row, (GRID_W, HD)), ref[0:GRID_W, :])
                )
            return jnp.concatenate(parts, axis=0)

        cosine = table(cos_ref)
        sine = table(sin_ref)
        even = lax.broadcasted_iota(jnp.int32, (tok, HD), 1) % 2 == 0
        rows = pl.ds(pl.multiple_of(slot * tok, tok), tok)
        for h in range(hq + hk):
            r = raw[:, h * HD : (h + 1) * HD]
            gain = gain_ref[0:1, :] if h < hq else gain_ref[1:2, :]
            n = r * lax.rsqrt(jnp.mean(r * r, axis=-1, keepdims=True) + EPS) * gain
            swapped = jnp.where(even, pltpu.roll(n, HD - 1, 1), pltpu.roll(n, 1, 1))
            turned = (n * cosine + swapped * sine).astype(jnp.bfloat16)
            if h < hq:
                q_s[h, rows, :] = turned
            else:
                k_s[h - hq, rows, :] = turned
        for h in range(hk):
            v_s[h, rows, :] = raw[:, (hq + hk + h) * HD : (hq + hk + h + 1) * HD].astype(
                jnp.bfloat16
            )

    for r in range(1, n_dp):
        w_copy(r, dp).start()
    for part in (0, 1):
        for kind in (0, 1):
            for way in (0, 1):
                ring_copy(way, part, kind, me, 0).start()
    spread(me)
    for r in range(1, n_dp):
        w_copy(r, lax.rem(dp - r + n_dp, n_dp)).wait_recv()
    project(me)

    @pl.loop(1, half)
    def _(t):
        for part in (0, 1):
            for kind in (0, 1):
                for way in (0, 1):
                    slot = slot_at(way, t)
                    ring_copy(way, part, kind, slot, t - 1).wait_recv()
                    if way == part:
                        ring_copy(way, part, kind, slot, t).start()
                    else:

                        @pl.when(t < half - 1)
                        def _():
                            ring_copy(way, part, kind, slot, t).start()

        for way in (0, 1):
            spread(slot_at(way, t))

        @pl.loop(0, 2)
        def _(way):
            project(slot_at(way, t))

    far = at_pos(pos + half)
    for kind in (0, 1):
        for way in (0, 1):
            ring_copy(way, way, kind, far, half - 1).wait_recv()
    spread(far)
    project(far)

    c = HD ** (-0.5) * LOG2E

    def att_copy(slot, source):
        return pltpu.make_async_remote_copy(
            src_ref=att_s.at[slot],
            dst_ref=att_all.at[source],
            send_sem=att_send.at[slot],
            recv_sem=att_recv.at[source],
            device_id={"sp": slot},
            device_id_type=MESH,
        )

    def attend(slot):
        rows = pl.ds(pl.multiple_of(slot * tok, tok), tok)
        for h in range(hq):
            g = h * hk // hq
            s = lax.dot_general(
                q_s[h, rows, :],
                k_s[g],
                (((1,), (1,)), ((), ())),
                preferred_element_type=jnp.float32,
            )
            p = jnp.exp2((s - jnp.max(s, axis=1, keepdims=True)) * c)
            inv = 1.0 / jnp.sum(p, axis=1, keepdims=True)
            probs = (p * inv).astype(jnp.bfloat16)
            att_s[slot, :, h * HD : (h + 1) * HD] = jnp.dot(
                probs, v_s[g], preferred_element_type=jnp.float32
            ).astype(jnp.bfloat16)

    @pl.loop(1, n_sp + 1)
    def _(r):
        slot = lax.rem(me + r, n_sp)
        attend(slot)

        @pl.when(r < n_sp)
        def _():
            att_copy(slot, me).start()

    att_all[me] = att_s[me]

    @pl.loop(1, n_sp)
    def _(r):
        source = lax.rem(me + r, n_sp)
        pltpu.make_async_remote_copy(
            src_ref=att_s.at[source],
            dst_ref=att_all.at[source],
            send_sem=att_send.at[source],
            recv_sem=att_recv.at[source],
            device_id={"sp": source},
            device_id_type=MESH,
        ).wait_recv()

    @pl.loop(0, n_sp)
    def _(slot):
        for r in range(1, n_dp):
            wo_copy(r, lax.rem(dp - r + n_dp, n_dp), slot).wait_recv()

    depth, cols = wo_all.shape[2], wo_all.shape[3]
    feat = hq * HD
    per = depth // feat

    @pl.loop(0, n_sp)
    def _(block):
        total = None
        for s in range(n_sp):
            term = jnp.dot(
                att_all[s],
                wo_all[s // per, block, (s % per) * feat : (s % per + 1) * feat, :],
                preferred_element_type=jnp.float32,
            )
            total = term if total is None else total + term
        out_ref[:, pl.ds(pl.multiple_of(block * cols, cols), cols)] = total.astype(out_ref.dtype)

    for r in range(1, n_dp):
        w_copy(r, dp).wait_send()

    @pl.loop(0, n_sp)
    def _(slot):
        for r in range(1, n_dp):
            wo_copy(r, dp, slot).wait_send()

    @pl.loop(0, half)
    def _(t):
        for part in (0, 1):
            for kind in (0, 1):
                for way in (0, 1):
                    if way == part:
                        ring_copy(way, part, kind, slot_at(way, t), t).wait_send()
                    else:

                        @pl.when(t < half - 1)
                        def _():
                            ring_copy(way, part, kind, slot_at(way, t), t).wait_send()

    @pl.loop(1, n_sp)
    def _(r):
        att_copy(lax.rem(me + r, n_sp), me).wait_send()


def on_device(tokens, w_query, w_key, w_value, w_out, qk_gain):
    n_sp = lax.axis_size("sp")
    n_dp = lax.axis_size("dp")
    own_rows = tokens[0]
    tok, width = own_rows.shape
    seq_len = tok * n_sp
    hq = HQ // n_sp
    hk = max(1, KV // n_sp)
    cosine, sine = rope_tables(seq_len)
    any_spec = pl.BlockSpec(memory_space=pl.ANY)
    vmem_spec = pl.BlockSpec(memory_space=pltpu.VMEM)
    half = n_sp // 2
    dma = pltpu.SemaphoreType.DMA
    bf16 = jnp.bfloat16
    out = pl.pallas_call(
        functools.partial(layer_kernel, n_sp, n_dp, hq, hk),
        out_shape=jax.ShapeDtypeStruct((tok, n_sp * w_out.shape[1]), bf16),
        in_specs=[any_spec] * 5 + [vmem_spec] * 3,
        out_specs=vmem_spec,
        scratch_shapes=[
            pltpu.VMEM((n_sp, tok, width), bf16),
            pltpu.VMEM((n_dp, w_query.shape[0], (hq + 2 * hk) * HD), bf16),
            pltpu.VMEM((n_dp, n_sp) + w_out.shape, bf16),
            pltpu.VMEM((hq, seq_len, HD), bf16),
            pltpu.VMEM((hk, seq_len, HD), bf16),
            pltpu.VMEM((hk, seq_len, HD), bf16),
            pltpu.VMEM((n_sp, tok, hq * HD), bf16),
            pltpu.VMEM((n_sp, tok, hq * HD), bf16),
            dma((5,)),
            dma((2, 2, 2, half)),
            dma((2, 2, 2, half)),
            dma((n_dp - 1,)),
            dma((n_dp - 1,)),
            dma((n_dp - 1, n_sp)),
            dma((n_dp - 1, n_sp)),
            dma((n_sp,)),
            dma((n_sp,)),
        ],
        compiler_params=pltpu.CompilerParams(
            collective_id=0, has_side_effects=True, vmem_limit_bytes=VMEM_CAP
        ),
    )(
        own_rows,
        w_query,
        head_columns(w_key, n_sp),
        head_columns(w_value, n_sp),
        w_out,
        cosine,
        sine,
        qk_gain,
    )
    return out[None]


def head_columns(weight, n_sp):
    local = weight.shape[1]
    if local >= HD:
        return weight
    group = HD // local
    groups = [list(range(g, g + group)) for g in range(0, n_sp, group)]
    return lax.all_gather(weight, "sp", axis=1, tiled=True, axis_index_groups=groups)


def solution(mesh):
    in_specs = (
        P("dp", "sp", None),
        P("dp", "sp"),
        P("dp", "sp"),
        P("dp", "sp"),
        P("dp", "sp"),
        P(),
    )
    return jax.shard_map(
        on_device, mesh=mesh, in_specs=in_specs, out_specs=P("dp", "sp", None), check_vma=False
    )
```

```python
import functools

import jax
import jax.numpy as jnp
from jax import lax
from jax.experimental import pallas as pl
from jax.experimental.pallas import tpu as pltpu
from jax.sharding import PartitionSpec as P

HQ = 16
KV = 8
HD = 128
GRID_W = 64
ROPE_BASE = 10000.0
EPS = 1e-06
LOG2E = 1.4426950408889634
VMEM_CAP = 60 * 1024 * 1024


MESH = pl.DeviceIdType.MESH


def rope_tables(seq_len):
    quarter = jnp.arange(0, HD // 2, 2, dtype=jnp.float32)
    inv_freq = jnp.repeat(ROPE_BASE ** (-quarter / (HD // 2)), 2)
    inv_freq = jnp.concatenate([inv_freq, inv_freq])
    count = max(GRID_W, seq_len // GRID_W)
    angle = jnp.arange(count, dtype=jnp.int32).astype(jnp.float32)[:, None] * inv_freq
    sign = jnp.where(jnp.arange(HD) % 2 == 0, -1.0, 1.0).astype(jnp.float32)
    return jnp.cos(angle), jnp.sin(angle) * sign


def layer_kernel(
    n_sp, n_dp, hq, hk,
    tok_ref, wq_ref, wk_ref, wv_ref, wo_ref, cos_ref, sin_ref, gain_ref,
    out_ref,
    x_all, w_all, wo_all, q_s, k_s, v_s, att_s, att_all,
    local_sem, ring_send, ring_recv, w_send, w_recv, wo_send, wo_recv, att_send, att_recv,
):
    tok = tok_ref.shape[0]
    half = n_sp // 2
    me = lax.axis_index("sp")
    dp = lax.axis_index("dp")
    pos = me // 2 + (me % 2) * (n_sp - 1 - 2 * (me // 2))

    def at_pos(p):
        p = lax.rem(p + 2 * n_sp, n_sp)
        return 2 * p + (p // half) * (2 * (n_sp - 1 - p) + 1 - 2 * p)

    q_cols, k_cols = wq_ref.shape[1], wk_ref.shape[1]
    mine = w_all.at[dp]
    loads = [
        (tok_ref, x_all.at[me]),
        (wo_ref, wo_all.at[dp, me]),
        (wq_ref, mine.at[:, 0:q_cols]),
        (wk_ref, mine.at[:, q_cols : q_cols + k_cols]),
        (wv_ref, mine.at[:, q_cols + k_cols : q_cols + 2 * k_cols]),
    ]
    loads = [pltpu.make_async_copy(a, b, local_sem.at[i]) for i, (a, b) in enumerate(loads)]
    for load in loads:
        load.start()

    barrier = pltpu.get_barrier_semaphore()
    for r in range(1, n_sp):
        pl.semaphore_signal(
            barrier, inc=1, device_id={"sp": lax.rem(me + r, n_sp)}, device_id_type=MESH
        )
    for r in range(1, n_dp):
        pl.semaphore_signal(
            barrier, inc=1, device_id={"dp": lax.rem(dp + r, n_dp)}, device_id_type=MESH
        )
    pl.semaphore_wait(barrier, n_sp - 1 + n_dp - 1)
    for load in loads:
        load.wait()

    def ring_copy(way, part, kind, slot, t):
        if kind == 0:
            rows = tok // 2
            ref = x_all.at[slot, part * rows : (part + 1) * rows]
        else:
            rows = wo_all.shape[2] // 2
            ref = wo_all.at[dp, slot, part * rows : (part + 1) * rows]
        return pltpu.make_async_remote_copy(
            src_ref=ref,
            dst_ref=ref,
            send_sem=ring_send.at[way, part, kind, t],
            recv_sem=ring_recv.at[way, part, kind, t],
            device_id={"sp": at_pos(pos + 1 - 2 * way)},
            device_id_type=MESH,
        )

    def slot_at(way, distance):
        return at_pos(pos - (1 - 2 * way) * distance)

    def w_copy(r, source):
        return pltpu.make_async_remote_copy(
            src_ref=w_all.at[source],
            dst_ref=w_all.at[source],
            send_sem=w_send.at[r - 1],
            recv_sem=w_recv.at[r - 1],
            device_id={"dp": lax.rem(dp + r, n_dp)},
            device_id_type=MESH,
        )

    def wo_copy(r, source, slot):
        return pltpu.make_async_remote_copy(
            src_ref=wo_all.at[source, slot],
            dst_ref=wo_all.at[source, slot],
            send_sem=wo_send.at[r - 1, slot],
            recv_sem=wo_recv.at[r - 1, slot],
            device_id={"dp": lax.rem(dp + r, n_dp)},
            device_id_type=MESH,
        )

    def spread(slot):
        for r in range(1, n_dp):
            wo_copy(r, dp, slot).start()

    def project(slot):
        raw = jnp.dot(
            x_all[slot],
            w_all[...].reshape(w_all.shape[0] * w_all.shape[1], w_all.shape[2]),
            preferred_element_type=jnp.float32,
        )
        lanes = lax.broadcasted_iota(jnp.int32, (GRID_W, HD), 1)
        grid_rows = tok // GRID_W

        def table(ref):
            parts = []
            for g in range(grid_rows):
                row = ref[pl.ds(slot * grid_rows + g, 1), :]
                parts.append(
                    jnp.where(lanes < HD // 2, jnp.broadcast_to(row, (GRID_W, HD)), ref[0:GRID_W, :])
                )
            return jnp.concatenate(parts, axis=0)

        cosine = table(cos_ref)
        sine = table(sin_ref)
        even = lax.broadcasted_iota(jnp.int32, (tok, HD), 1) % 2 == 0
        rows = pl.ds(pl.multiple_of(slot * tok, tok), tok)
        for h in range(hq + hk):
            r = raw[:, h * HD : (h + 1) * HD]
            gain = gain_ref[0:1, :] if h < hq else gain_ref[1:2, :]
            n = r * lax.rsqrt(jnp.mean(r * r, axis=-1, keepdims=True) + EPS) * gain
            swapped = jnp.where(even, pltpu.roll(n, HD - 1, 1), pltpu.roll(n, 1, 1))
            turned = (n * cosine + swapped * sine).astype(jnp.bfloat16)
            if h < hq:
                q_s[h, rows, :] = turned
            else:
                k_s[h - hq, rows, :] = turned
        for h in range(hk):
            v_s[h, rows, :] = raw[:, (hq + hk + h) * HD : (hq + hk + h + 1) * HD].astype(
                jnp.bfloat16
            )

    for r in range(1, n_dp):
        w_copy(r, dp).start()
    for kind in (0, 1):
        for part in (0, 1):
            for way in (0, 1):
                ring_copy(way, part, kind, me, 0).start()
    spread(me)
    for r in range(1, n_dp):
        w_copy(r, lax.rem(dp - r + n_dp, n_dp)).wait_recv()
    project(me)

    @pl.loop(1, half)
    def _(t):
        for kind in (0, 1):
            for part in (0, 1):
                for way in (0, 1):
                    slot = slot_at(way, t)
                    ring_copy(way, part, kind, slot, t - 1).wait_recv()
                    if way == part:
                        ring_copy(way, part, kind, slot, t).start()
                    else:

                        @pl.when(t < half - 1)
                        def _():
                            ring_copy(way, part, kind, slot, t).start()

        for way in (0, 1):
            spread(slot_at(way, t))

        @pl.loop(0, 2)
        def _(way):
            project(slot_at(way, t))

    far = at_pos(pos + half)
    for way in (0, 1):
        ring_copy(way, way, 0, far, half - 1).wait_recv()
    project(far)
    for way in (0, 1):
        ring_copy(way, way, 1, far, half - 1).wait_recv()
    spread(far)

    c = HD ** (-0.5) * LOG2E

    def att_copy(slot, source):
        return pltpu.make_async_remote_copy(
            src_ref=att_s.at[slot],
            dst_ref=att_all.at[source],
            send_sem=att_send.at[slot],
            recv_sem=att_recv.at[source],
            device_id={"sp": slot},
            device_id_type=MESH,
        )

    def attend(slot):
        rows = pl.ds(pl.multiple_of(slot * tok, tok), tok)
        for h in range(hq):
            g = h * hk // hq
            s = lax.dot_general(
                q_s[h, rows, :],
                k_s[g],
                (((1,), (1,)), ((), ())),
                preferred_element_type=jnp.float32,
            )
            p = jnp.exp2((s - jnp.max(s, axis=1, keepdims=True)) * c)
            inv = 1.0 / jnp.sum(p, axis=1, keepdims=True)
            probs = (p * inv).astype(jnp.bfloat16)
            att_s[slot, :, h * HD : (h + 1) * HD] = jnp.dot(
                probs, v_s[g], preferred_element_type=jnp.float32
            ).astype(jnp.bfloat16)

    @pl.loop(1, n_sp + 1)
    def _(r):
        slot = lax.rem(me + r, n_sp)
        attend(slot)

        @pl.when(r < n_sp)
        def _():
            att_copy(slot, me).start()

    att_all[me] = att_s[me]

    @pl.loop(1, n_sp)
    def _(r):
        source = lax.rem(me + r, n_sp)
        pltpu.make_async_remote_copy(
            src_ref=att_s.at[source],
            dst_ref=att_all.at[source],
            send_sem=att_send.at[source],
            recv_sem=att_recv.at[source],
            device_id={"sp": source},
            device_id_type=MESH,
        ).wait_recv()

    @pl.loop(0, n_sp)
    def _(slot):
        for r in range(1, n_dp):
            wo_copy(r, lax.rem(dp - r + n_dp, n_dp), slot).wait_recv()

    depth, cols = wo_all.shape[2], wo_all.shape[3]
    feat = hq * HD
    per = depth // feat

    @pl.loop(0, n_sp)
    def _(block):
        total = None
        for s in range(n_sp):
            term = jnp.dot(
                att_all[s],
                wo_all[s // per, block, (s % per) * feat : (s % per + 1) * feat, :],
                preferred_element_type=jnp.float32,
            )
            total = term if total is None else total + term
        out_ref[:, pl.ds(pl.multiple_of(block * cols, cols), cols)] = total.astype(out_ref.dtype)

    for r in range(1, n_dp):
        w_copy(r, dp).wait_send()

    @pl.loop(0, n_sp)
    def _(slot):
        for r in range(1, n_dp):
            wo_copy(r, dp, slot).wait_send()

    @pl.loop(0, half)
    def _(t):
        for part in (0, 1):
            for kind in (0, 1):
                for way in (0, 1):
                    if way == part:
                        ring_copy(way, part, kind, slot_at(way, t), t).wait_send()
                    else:

                        @pl.when(t < half - 1)
                        def _():
                            ring_copy(way, part, kind, slot_at(way, t), t).wait_send()

    @pl.loop(1, n_sp)
    def _(r):
        att_copy(lax.rem(me + r, n_sp), me).wait_send()


def on_device(tokens, w_query, w_key, w_value, w_out, qk_gain):
    n_sp = lax.axis_size("sp")
    n_dp = lax.axis_size("dp")
    own_rows = tokens[0]
    tok, width = own_rows.shape
    seq_len = tok * n_sp
    hq = HQ // n_sp
    hk = max(1, KV // n_sp)
    cosine, sine = rope_tables(seq_len)
    any_spec = pl.BlockSpec(memory_space=pl.ANY)
    vmem_spec = pl.BlockSpec(memory_space=pltpu.VMEM)
    half = n_sp // 2
    dma = pltpu.SemaphoreType.DMA
    bf16 = jnp.bfloat16
    out = pl.pallas_call(
        functools.partial(layer_kernel, n_sp, n_dp, hq, hk),
        out_shape=jax.ShapeDtypeStruct((tok, n_sp * w_out.shape[1]), bf16),
        in_specs=[any_spec] * 5 + [vmem_spec] * 3,
        out_specs=vmem_spec,
        scratch_shapes=[
            pltpu.VMEM((n_sp, tok, width), bf16),
            pltpu.VMEM((n_dp, w_query.shape[0], (hq + 2 * hk) * HD), bf16),
            pltpu.VMEM((n_dp, n_sp) + w_out.shape, bf16),
            pltpu.VMEM((hq, seq_len, HD), bf16),
            pltpu.VMEM((hk, seq_len, HD), bf16),
            pltpu.VMEM((hk, seq_len, HD), bf16),
            pltpu.VMEM((n_sp, tok, hq * HD), bf16),
            pltpu.VMEM((n_sp, tok, hq * HD), bf16),
            dma((5,)),
            dma((2, 2, 2, half)),
            dma((2, 2, 2, half)),
            dma((n_dp - 1,)),
            dma((n_dp - 1,)),
            dma((n_dp - 1, n_sp)),
            dma((n_dp - 1, n_sp)),
            dma((n_sp,)),
            dma((n_sp,)),
        ],
        compiler_params=pltpu.CompilerParams(
            collective_id=0, has_side_effects=True, vmem_limit_bytes=VMEM_CAP
        ),
    )(
        own_rows,
        w_query,
        head_columns(w_key, n_sp),
        head_columns(w_value, n_sp),
        w_out,
        cosine,
        sine,
        qk_gain,
    )
    return out[None]


def head_columns(weight, n_sp):
    local = weight.shape[1]
    if local >= HD:
        return weight
    group = HD // local
    groups = [list(range(g, g + group)) for g in range(0, n_sp, group)]
    return lax.all_gather(weight, "sp", axis=1, tiled=True, axis_index_groups=groups)


def solution(mesh):
    in_specs = (
        P("dp", "sp", None),
        P("dp", "sp"),
        P("dp", "sp"),
        P("dp", "sp"),
        P("dp", "sp"),
        P(),
    )
    return jax.shard_map(
        on_device, mesh=mesh, in_specs=in_specs, out_specs=P("dp", "sp", None), check_vma=False
    )
```
